32 devices in a mesh: vp: 8 (over z, x), dp: 4 (over y, core).
Axes of the slice: x: 2, y: 2, z: 4, core: 2. Of those that a mesh axis runs over, the one named last changes fastest.
Arguments:
- hidden_rows: bfloat16 [768, 4, 2048], P('vp', 'dp'), may hold values from -48 to 48
- norm_gain: float32 [2048], replicated, may hold values from 0.1 to 1.9
- vocab_matrix: bfloat16 [2048, 8192], P(None, 'vp'), may hold values from -3 to 3
- vocab_bias: float32 [8192], P('vp'), may hold values from -4 to 4
- targets: int32 [768, 4], P(None, 'dp'), may hold values from 0 to 8191
- loss_weight: float32 [768, 4], P(None, 'dp'), may hold values from 0.5 to 8
Outputs:
- losses: float32 [768, 4], P('vp', 'dp')
- norm_grad: float32 [768, 4, 2048], P('vp', 'dp')
- vocab_grad: float32 [2048, 8192], P('dp', 'vp')
The draws below stay inside these ranges and needn't reach their ends.
All inputs are finite; a program needn't handle non-finite values.
Results may differ from the reference program's by a relative error of at most 0.0056.
Values may be sent and summed in bfloat16 or wider, within the bound.
A program may use at most 64 MiB of HBM per device.

```python
import math
import jax
import jax.numpy as jnp
import numpy as np
from jax import lax

D = 2048
V_DEV = 1024
TOK_DEV = 768
VOCAB = 8192
TOKENS = 3072
N_DP = 4


def draw_vocab_matrix(key, part):
    matrix = jnp.clip(jax.random.normal(jax.random.fold_in(key, 21), (D, VOCAB), jnp.float32), -6.0, 6.0) * (2.5 / math.sqrt(D))
    return matrix.astype(jnp.bfloat16)


def draw_hidden_rows(key, part):
    inputs = jnp.clip(jax.random.normal(jax.random.fold_in(key, 31), (TOKENS, D), jnp.float32), -6.0, 6.0)
    return inputs.reshape(TOK_DEV, TOKENS // TOK_DEV, D).astype(jnp.bfloat16)


def draw_vocab_bias(key, part):
    shard_ids = jnp.arange(VOCAB, dtype=jnp.int32) // V_DEV
    levels = jax.random.uniform(jax.random.fold_in(key, 41), (VOCAB // V_DEV,), jnp.float32, -1.5, 1.5)
    noise = 0.5 * jnp.clip(jax.random.normal(jax.random.fold_in(key, 42), (VOCAB,), jnp.float32), -4.0, 4.0)
    return levels[shard_ids] + noise


def place_ends(result, rng, smallest, high):
    index_at = [jax.random.randint(jax.random.fold_in(rng, axis), (), 0, length) for axis, length in enumerate(result.shape)]
    longest = result.shape.index(max(result.shape))
    neighbour = index_at[:longest] + [(index_at[longest] + 1) % result.shape[longest]] + index_at[longest + 1:]
    return result.at[tuple(index_at)].set(smallest).at[tuple(neighbour)].set(high)


def block_scale(own_key, extent, cuts, low, top_value):
    level = 1.0
    for dim, blocks in cuts:
        heights = jax.random.uniform(jax.random.fold_in(jax.random.fold_in(own_key, 6), dim), (blocks,), jnp.float32, low / len(cuts), top_value / len(cuts))
        level = level * jnp.repeat(jnp.exp(heights), extent[dim] // blocks).reshape((-1,) + (1,) * (len(extent) - 1 - dim))
    return level


def rank_bounds(amount, skew):
    weights = [(1 << 20) // math.isqrt(grade ** skew) + 1 for grade in range(1, amount + 1)]
    deviation = 1 + sum(weights) // (1 << 30)
    return np.cumsum(np.array([max(1, weight // deviation) for weight in weights]))


def ranked(key, dims, amount, skew):
    grid = rank_bounds(amount, skew)
    pick = jax.random.randint(jax.random.fold_in(key, 1), dims, 0, int(grid[amount - 1]))
    grade = jnp.searchsorted(jnp.asarray(grid, jnp.int32), pick, side="right")
    return jax.random.permutation(jax.random.fold_in(key, 2), amount)[grade].astype(jnp.int32)


def setup_inputs(seed: int = 0) -> dict:
    arg_keys = jax.random.split(jax.random.key(seed), 7)
    hidden_rows = draw_hidden_rows(jax.random.fold_in(arg_keys[6], 71), 0)
    norm_gain = jnp.clip(1.0 + 0.18 * jax.random.normal(arg_keys[1], (D,), jnp.float32), 0.1, 1.9)
    vocab_matrix = draw_vocab_matrix(jax.random.fold_in(arg_keys[6], 71), 0)
    vocab_bias = draw_vocab_bias(jax.random.fold_in(arg_keys[6], 71), 0)
    targets = place_ends(ranked(arg_keys[4], (TOK_DEV, N_DP), VOCAB, 2), jax.random.fold_in(arg_keys[4], 3), 0, VOCAB - 1).astype(jnp.int32)
    loss_weight = jnp.clip(jnp.exp(math.log(8.0) - 2.7725887 * jax.random.uniform(arg_keys[5], (TOK_DEV, N_DP), jnp.float32) ** block_scale(arg_keys[5], (TOK_DEV, N_DP), ((1, 4),), -0.2, 0.2)), 0.5, 8.0)
    return {"hidden_rows": hidden_rows, "norm_gain": norm_gain, "vocab_matrix": vocab_matrix, "vocab_bias": vocab_bias, "targets": targets, "loss_weight": loss_weight}


epsilon = 1e-06
penalty = 0.005

def reference(hidden_rows, norm_gain, vocab_matrix, vocab_bias, targets, loss_weight):
    inputs = hidden_rows.astype(jnp.float32)
    inverse_rms = lax.rsqrt(lax.optimization_barrier(jnp.mean(inputs * inputs, axis=-1, keepdims=True)) + epsilon)
    unit_rows = inputs * inverse_rms
    normed = (unit_rows * norm_gain).astype(jnp.bfloat16)
    column_ids = jnp.arange(VOCAB, dtype=jnp.int32)

    def one_group(carry, group):
        row_block, target_ids, weights = group
        scores = jnp.dot(row_block, vocab_matrix, preferred_element_type=jnp.float32) + vocab_bias[None, :]
        maxima = lax.optimization_barrier(jnp.max(scores, axis=1))
        totals = lax.optimization_barrier(jnp.sum(jnp.exp(scores - maxima[:, None]), axis=1))
        log_total = maxima + jnp.log(totals)
        is_target = column_ids[None, :] == target_ids[:, None]
        target_score = lax.optimization_barrier(jnp.sum(jnp.where(is_target, scores, 0.0), axis=1))
        loss_rows = log_total - target_score + penalty * log_total * log_total
        probs = jnp.exp(scores - log_total[:, None])
        score_grad = (weights[:, None] * ((1.0 + 2.0 * penalty * log_total)[:, None] * probs - jnp.where(is_target, 1.0, 0.0))).astype(jnp.bfloat16)
        row_grad = lax.dot_general(score_grad, vocab_matrix, (((1,), (1,)), ((), ())), preferred_element_type=jnp.float32)
        carry = carry + jnp.dot(row_block.T, score_grad, preferred_element_type=jnp.float32)
        return (carry, (loss_rows, row_grad))
    groups = (jnp.moveaxis(normed, 1, 0), targets.T, loss_weight.T)
    vocab_grad, (loss_groups, grad_groups) = lax.scan(one_group, jnp.zeros((D, VOCAB), jnp.float32), groups)
    row_grad = jnp.moveaxis(grad_groups, 0, 1)
    scaled_grad = norm_gain * row_grad
    norm_grad = inverse_rms * (scaled_grad - unit_rows * lax.optimization_barrier(jnp.mean(scaled_grad * unit_rows, axis=-1, keepdims=True)))
    return (loss_groups.T, norm_grad, vocab_grad)
```

```python
import functools

import jax
import jax.numpy as jnp
from jax import lax
from jax.experimental import pallas as pl
from jax.experimental.pallas import tpu as pltpu
from jax.sharding import PartitionSpec as P

epsilon = 1e-06
penalty = 0.005
MESH = pl.DeviceIdType.MESH
CHUNKS = 2


def kernel(
    n, nx, ny,
    hid_ref, gain_ref, mat_hbm, bias_ref, tgt_ref, wgt_ref,
    loss_ref, ngrad_ref, vout_ref,
    rows, mat, scores, sg, part, xsend, xrecv, zsend, zrecv,
    rowst, csend, crecv, ysend, yrecv, own, statc, stats_out, stats_all, colv,
    mat_sem, ag_r, ag_up, ag_dn, ag_x, st_s, st_r, xs, xr, zs, zr, cs, cr, ys, yr,
):
    nz = n // nx
    me = lax.axis_index("vp")
    dme = lax.axis_index("dp")
    z, x = me // nx, me % nx
    y, core = dme // 2, dme % 2
    own_rows, width = hid_ref.shape
    columns = mat.shape[1]
    total = n * own_rows
    half = width // CHUNKS
    out_rows = vout_ref.shape[0]
    f32, bf16 = jnp.float32, jnp.bfloat16

    mat_copy = pltpu.make_async_copy(mat_hbm, mat, mat_sem)
    mat_copy.start()

    barrier = pltpu.get_barrier_semaphore()

    def greet(k, _):
        pl.semaphore_signal(barrier, inc=1, device_id={"vp": (me + k) % n}, device_id_type=MESH)
        return 0

    lax.fori_loop(1, n, greet, 0)
    partner = y * 2 + 1 - core
    pl.semaphore_signal(barrier, inc=1, device_id={"dp": partner}, device_id_type=MESH)
    for q in range(ny - 1):
        pl.semaphore_signal(
            barrier, inc=1, device_id={"dp": ((y + 1 + q) % ny) * 2 + core}, device_id_type=MESH
        )

    hid = hid_ref[...].astype(f32)
    inverse_rms = lax.rsqrt(jnp.mean(hid * hid, axis=-1, keepdims=True) + epsilon)
    rows[me] = (hid * inverse_rms * gain_ref[...]).astype(bf16)
    pl.semaphore_wait(barrier, n - 1 + ny)

    def ag_copy(b, h, send_sem, target):
        piece = rows.at[b, :, pl.ds(h * half, half)]
        return pltpu.make_async_remote_copy(
            src_ref=piece, dst_ref=piece, send_sem=send_sem, recv_sem=ag_r.at[b * CHUNKS + h],
            device_id={"vp": target}, device_id_type=MESH,
        )

    def up_copy(zz, h):
        return ag_copy(zz * nx + x, h, ag_up.at[zz * CHUNKS + h], (z + 1) * nx + x)

    def down_copy(zz, h):
        return ag_copy(zz * nx + x, h, ag_dn.at[zz * CHUNKS + h], (z - 1) * nx + x)

    def x_copy(zz, h, j):
        return ag_copy(
            zz * nx + x, h, ag_x.at[((j - 1) * nz + zz) * CHUNKS + h], z * nx + (x + j) % nx
        )

    def got(b, h):
        ag_copy(b, h, ag_up.at[0], (me + 1) % n).wait_recv()

    def forward(k, h):
        below, above = z - k, z + k

        @pl.when(below >= 0)
        def _():
            @pl.when(k > 0)
            def _():
                got(below * nx + x, h)

            @pl.when(z < nz - 1)
            def _():
                up_copy(below, h).start()

            @pl.when((k == 0) & (z > 0))
            def _():
                down_copy(below, h).start()

            for j in range(1, nx):
                x_copy(below, h, j).start()

        @pl.when((k > 0) & (above < nz))
        def _():
            got(above * nx + x, h)

            @pl.when(z > 0)
            def _():
                down_copy(above, h).start()

            for j in range(1, nx):
                x_copy(above, h, j).start()

    lanes = lax.broadcasted_iota(jnp.int32, (own_rows, 128), 1)
    column_ids = lax.broadcasted_iota(jnp.int32, (own_rows, columns), 1)

    def score(b):
        s = jnp.dot(rows[b], mat[...], preferred_element_type=f32) + bias_ref[...]
        scores[b] = s
        m = jnp.max(s, axis=1, keepdims=True)
        t = jnp.sum(jnp.exp(s - m), axis=1, keepdims=True)
        hit = column_ids == tgt_ref[b] - me * columns
        g = jnp.sum(jnp.where(hit, s, 0.0), axis=1, keepdims=True)
        statc[b] = jnp.where(lanes == 0, m, jnp.where(lanes == 1, t, g))

    def gather_step(k, _):
        @pl.when(k < nz)
        def _():
            for h in range(CHUNKS):
                forward(k, h)

        @pl.when(k == 0)
        def _():
            mat_copy.wait()

        def visit(t, _):
            i, j = t % 2, t // 2
            kk = jnp.where(j == 0, k, k - 1)
            zz = z + (2 * i - 1) * kk
            b = zz * nx + (x + j) % nx

            @pl.when((kk >= 0) & (zz >= 0) & (zz < nz) & ((kk > 0) | (i == 0)))
            def _():
                @pl.when(j > 0)
                def _():
                    for h in range(CHUNKS):
                        got(b, h)

                score(b)

            return 0

        lax.fori_loop(0, 2 * nx, visit, 0)
        return 0

    lax.fori_loop(0, nz + 1, gather_step, 0)

    packed = jnp.transpose(statc[...].reshape(total, 128))[0:8]
    stats_out[...] = packed
    stats_all[0] = packed

    def stat_copy(k):
        return pltpu.make_async_remote_copy(
            src_ref=stats_out, dst_ref=stats_all.at[k], send_sem=st_s.at[k], recv_sem=st_r.at[k],
            device_id={"vp": (me + k) % n}, device_id_type=MESH,
        )

    def stat_start(k, _):
        stat_copy(k).start()
        return 0

    lax.fori_loop(1, n, stat_start, 0)

    def turn(c, _):
        at = pl.ds(pl.multiple_of(c * 128, 128), 128)
        rowst[at, :] = jnp.transpose(rows[:, :, at].astype(f32).reshape(total, 128)).astype(bf16)
        return 0

    lax.fori_loop(0, width // 128, turn, 0)

    def stat_wait(k, _):
        stat_copy(k).wait()
        return 0

    lax.fori_loop(1, n, stat_wait, 0)
    every = stats_all[...]
    peak = jnp.max(every[:, 0:1, :], axis=0)
    summed = jnp.sum(every[:, 1:2, :] * jnp.exp(every[:, 0:1, :] - peak[None]), axis=0)
    hit_score = jnp.sum(every[:, 2:3, :], axis=0)
    log_total = peak + jnp.log(summed)
    loss = log_total - hit_score + penalty * log_total * log_total
    stacked = jnp.concatenate([log_total, loss, jnp.zeros((126, total), f32)], axis=0)
    colv[...] = jnp.transpose(stacked).reshape(n, own_rows, 128)
    loss_ref[...] = colv[me][:, 1:2]

    def grads(b, _):
        lt = colv[b][:, 0:1]
        w = wgt_ref[b]
        hit = column_ids == tgt_ref[b] - me * columns
        probs = jnp.exp(scores[b] - lt)
        sg[b] = (
            w * ((1.0 + 2.0 * penalty * lt) * probs - jnp.where(hit, 1.0, 0.0))
        ).astype(bf16)
        return 0

    lax.fori_loop(0, n, grads, 0)

    def x_send(slot, j):
        return pltpu.make_async_remote_copy(
            src_ref=xsend.at[slot], dst_ref=xrecv.at[slot], send_sem=xs.at[slot], recv_sem=xr.at[slot],
            device_id={"vp": z * nx + (x + j) % nx}, device_id_type=MESH,
        )

    def row_part(u, _):
        j = (u // (2 * nz) + 1) % nx
        k = nz - 1 - (u // 2) % nz
        i = u % 2
        zz = z + (2 * i - 1) * k

        @pl.when((zz >= 0) & (zz < nz) & ((k > 0) | (i == 0)))
        def _():
            b = zz * nx + (x + j) % nx
            p = lax.dot_general(sg[b], mat[...], (((1,), (1,)), ((), ())), preferred_element_type=f32)

            @pl.when(j > 0)
            def _():
                slot = (j - 1) * nz + zz
                xsend[slot] = p.astype(bf16)
                x_send(slot, j).start()

            @pl.when(j == 0)
            def _():
                part[zz] = p

        return 0

    def flat_grad():
        if own_rows % 16 == 0:
            return sg[...].reshape(total, columns)
        return sg[...].astype(f32).reshape(total, columns).astype(bf16)

    def vocab_part(d):
        at = pl.ds(pl.multiple_of(d * out_rows, out_rows), out_rows)
        return jnp.dot(rowst[at, :], flat_grad(), preferred_element_type=f32)

    def core_copy(q):
        return pltpu.make_async_remote_copy(
            src_ref=csend.at[q], dst_ref=crecv.at[q], send_sem=cs.at[q], recv_sem=cr.at[q],
            device_id={"dp": partner}, device_id_type=MESH,
        )

    def y_copy(q):
        return pltpu.make_async_remote_copy(
            src_ref=ysend.at[q], dst_ref=yrecv.at[q], send_sem=ys.at[q], recv_sem=yr.at[q],
            device_id={"dp": ((y + 1 + q) % ny) * 2 + core}, device_id_type=MESH,
        )

    def core_part(q, _):
        csend[q] = vocab_part(((y + 1 + q) % ny) * 2 + 1 - core).astype(bf16)
        core_copy(q).start()
        return 0

    def own_part(q, _):
        own[...] = vocab_part(((y + 1 + q) % ny) * 2 + core)
        core_copy(q).wait_recv()

        @pl.when(q < ny - 1)
        def _():
            slot = jnp.minimum(q, max(ny - 2, 0))
            ysend[slot] = (own[...] + crecv[q].astype(f32)).astype(bf16)
            y_copy(slot).start()

        @pl.when(q == ny - 1)
        def _():
            vout_ref[...] = own[...] + crecv[q].astype(f32)

        return 0

    def z_copy(i, zz):
        return pltpu.make_async_remote_copy(
            src_ref=zsend.at[zz], dst_ref=zrecv.at[i * nz + zz], send_sem=zs.at[zz],
            recv_sem=zr.at[i * nz + zz],
            device_id={"vp": (z + 2 * i - 1) * nx + x}, device_id_type=MESH,
        )

    def add_x(zz):
        for j in range(1, nx):
            slot = (j - 1) * nz + zz
            x_send(slot, j).wait_recv()
            part[zz] += xrecv[slot].astype(f32)

    def add_z(i, zz):
        z_copy(i, zz).wait_recv()
        part[zz] += zrecv[i * nz + zz].astype(f32)

    def chain(k):
        def one(i, _):
            zz = z + (2 * i - 1) * k

            @pl.when((zz >= 0) & (zz < nz))
            def _():
                add_x(zz)

                @pl.when(((i == 1) & (z > 0)) | ((i == 0) & (z < nz - 1)))
                def _():
                    add_z(i, zz)

                zsend[zz] = part[zz].astype(bf16)
                z_copy(i, zz).start()

            return 0

        lax.fori_loop(0, 2, one, 0)

    def chain_at(s, _):
        chain(nz - 1 - s)
        return 0

    lax.fori_loop(0, 2 * nz * (nx - 1), row_part, 0)
    lax.fori_loop(0, ny, core_part, 0)
    lax.fori_loop(2 * nz * (nx - 1), 2 * nz * nx, row_part, 0)
    lax.fori_loop(0, 1, chain_at, 0)
    lax.fori_loop(0, ny, own_part, 0)
    lax.fori_loop(1, nz - 1, chain_at, 0)

    add_x(z)

    @pl.when(z > 0)
    def _():
        add_z(1, z)

    @pl.when(z < nz - 1)
    def _():
        add_z(0, z)

    hid = hid_ref[...].astype(f32)
    inverse_rms = lax.rsqrt(jnp.mean(hid * hid, axis=-1, keepdims=True) + epsilon)
    unit = hid * inverse_rms
    scaled = gain_ref[...] * part[z]
    ngrad_ref[...] = inverse_rms * (scaled - unit * jnp.mean(scaled * unit, axis=-1, keepdims=True))

    for q in range(ny - 1):
        y_copy(q).wait_recv()
        vout_ref[...] += yrecv[q].astype(f32)

    def drain(zz, _):
        for h in range(CHUNKS):
            @pl.when((zz <= z) & (z < nz - 1))
            def _():
                up_copy(zz, h).wait_send()

            @pl.when((zz >= z) & (z > 0))
            def _():
                down_copy(zz, h).wait_send()

            for j in range(1, nx):
                x_copy(zz, h, j).wait_send()

        for j in range(1, nx):
            x_send((j - 1) * nz + zz, j).wait_send()

        @pl.when(zz > z)
        def _():
            z_copy(1, zz).wait_send()

        @pl.when(zz < z)
        def _():
            z_copy(0, zz).wait_send()

        return 0

    lax.fori_loop(0, nz, drain, 0)
    for q in range(ny):
        core_copy(q).wait_send()
    for q in range(ny - 1):
        y_copy(q).wait_send()


def solution(mesh):
    n, dp = mesh.shape["vp"], mesh.shape["dp"]
    ny = dp // 2
    nx = 1
    while (2 * nx) ** 2 <= n and n % (2 * nx) == 0:
        nx *= 2
    nz = n // nx

    def local(hidden_rows, norm_gain, vocab_matrix, vocab_bias, targets, loss_weight):
        own_rows, _, width = hidden_rows.shape
        columns = vocab_matrix.shape[1]
        total = n * own_rows
        out_rows = width // dp
        f32, bf16 = jnp.float32, jnp.bfloat16
        vmem = pl.BlockSpec(memory_space=pltpu.VMEM)
        dma = pltpu.SemaphoreType.DMA
        others = max(ny - 1, 1)
        xslots = max((nx - 1) * nz, 1)
        block = (own_rows, width)
        losses, norm_grad, vocab_grad = pl.pallas_call(
            functools.partial(kernel, n, nx, ny),
            out_shape=(
                jax.ShapeDtypeStruct((own_rows, 1), f32),
                jax.ShapeDtypeStruct(block, f32),
                jax.ShapeDtypeStruct((out_rows, columns), f32),
            ),
            in_specs=[vmem, vmem, pl.BlockSpec(memory_space=pl.ANY), vmem, vmem, vmem],
            out_specs=(vmem, vmem, vmem),
            scratch_shapes=[
                pltpu.VMEM((n,) + block, bf16),
                pltpu.VMEM((width, columns), bf16),
                pltpu.VMEM((n, own_rows, columns), f32),
                pltpu.VMEM((n, own_rows, columns), bf16),
                pltpu.VMEM((nz,) + block, f32),
                pltpu.VMEM((xslots,) + block, bf16),
                pltpu.VMEM((xslots,) + block, bf16),
                pltpu.VMEM((nz,) + block, bf16),
                pltpu.VMEM((2 * nz,) + block, bf16),
                pltpu.VMEM((width, total), bf16),
                pltpu.VMEM((ny, out_rows, columns), bf16),
                pltpu.VMEM((ny, out_rows, columns), bf16),
                pltpu.VMEM((others, out_rows, columns), bf16),
                pltpu.VMEM((others, out_rows, columns), bf16),
                pltpu.VMEM((out_rows, columns), f32),
                pltpu.VMEM((n, own_rows, 128), f32),
                pltpu.VMEM((8, total), f32),
                pltpu.VMEM((n, 8, total), f32),
                pltpu.VMEM((n, own_rows, 128), f32),
                dma,
                dma((n * CHUNKS,)),
                dma((nz * CHUNKS,)),
                dma((nz * CHUNKS,)),
                dma((xslots * CHUNKS,)),
                dma((n,)),
                dma((n,)),
                dma((xslots,)),
                dma((xslots,)),
                dma((nz,)),
                dma((2 * nz,)),
                dma((ny,)),
                dma((ny,)),
                dma((others,)),
                dma((others,)),
            ],
            compiler_params=pltpu.CompilerParams(
                collective_id=0, has_side_effects=True, vmem_limit_bytes=60 * 1024 * 1024
            ),
        )(
            hidden_rows.reshape(block),
            norm_gain.reshape(1, width),
            vocab_matrix,
            vocab_bias.reshape(1, columns),
            targets.reshape(n, own_rows, 1),
            loss_weight.reshape(n, own_rows, 1),
        )
        return losses, norm_grad.reshape(own_rows, 1, width), vocab_grad

    in_specs = (P("vp", "dp", None), P(), P(None, "vp"), P("vp"), P(None, "dp"), P(None, "dp"))
    out_specs = (P("vp", "dp"), P("vp", "dp", None), P("dp", "vp"))
    return jax.shard_map(local, mesh=mesh, in_specs=in_specs, out_specs=out_specs, check_vma=False)
```

```python
import functools

import jax
import jax.numpy as jnp
from jax import lax
from jax.experimental import pallas as pl
from jax.experimental.pallas import tpu as pltpu
from jax.sharding import PartitionSpec as P

epsilon = 1e-06
penalty = 0.005
MESH = pl.DeviceIdType.MESH
CHUNKS = 2


def kernel(
    n, nx, ny,
    hid_ref, gain_ref, mat_hbm, bias_ref, tgt_ref, wgt_ref,
    loss_ref, ngrad_ref, vout_ref,
    rows, mat, scores, sg, part, xsend, xrecv, zsend, zrecv,
    rowst, csend, crecv, ysend, yrecv, own, statc, stats_out, stats_all, colv, tw,
    mat_sem, ag_r, ag_up, ag_dn, ag_x, st_s, st_r, xs, xr, zs, zr, cs, cr, ys, yr,
):
    nz = n // nx
    me = lax.axis_index("vp")
    dme = lax.axis_index("dp")
    z, x = me // nx, me % nx
    y, core = dme // 2, dme % 2
    own_rows, width = hid_ref.shape
    columns = mat.shape[1]
    total = n * own_rows
    half = width // CHUNKS
    out_rows = vout_ref.shape[0]
    f32, bf16 = jnp.float32, jnp.bfloat16

    mat_copy = pltpu.make_async_copy(mat_hbm, mat, mat_sem)
    mat_copy.start()

    barrier = pltpu.get_barrier_semaphore()

    def greet(k, _):
        pl.semaphore_signal(barrier, inc=1, device_id={"vp": (me + k) % n}, device_id_type=MESH)
        return 0

    lax.fori_loop(1, n, greet, 0)
    partner = y * 2 + 1 - core
    pl.semaphore_signal(barrier, inc=1, device_id={"dp": partner}, device_id_type=MESH)
    for q in range(ny - 1):
        pl.semaphore_signal(
            barrier, inc=1, device_id={"dp": ((y + 1 + q) % ny) * 2 + core}, device_id_type=MESH
        )

    hid = hid_ref[...].astype(f32)
    inverse_rms = lax.rsqrt(jnp.mean(hid * hid, axis=-1, keepdims=True) + epsilon)
    rows[me] = (hid * inverse_rms * gain_ref[...]).astype(bf16)
    turned = jnp.transpose(
        jnp.concatenate(
            [
                (tgt_ref[...] - me * columns).astype(f32),
                wgt_ref[...],
                jnp.zeros((126, total), f32),
            ],
            axis=0,
        )
    )
    tw[...] = turned.reshape(n, own_rows, 128)
    pl.semaphore_wait(barrier, n - 1 + ny)

    def ag_copy(b, h, send_sem, target):
        piece = rows.at[b, :, pl.ds(h * half, half)]
        return pltpu.make_async_remote_copy(
            src_ref=piece, dst_ref=piece, send_sem=send_sem, recv_sem=ag_r.at[b * CHUNKS + h],
            device_id={"vp": target}, device_id_type=MESH,
        )

    def up_copy(zz, h):
        return ag_copy(zz * nx + x, h, ag_up.at[zz * CHUNKS + h], (z + 1) * nx + x)

    def down_copy(zz, h):
        return ag_copy(zz * nx + x, h, ag_dn.at[zz * CHUNKS + h], (z - 1) * nx + x)

    def x_copy(zz, h, j):
        return ag_copy(
            zz * nx + x, h, ag_x.at[((j - 1) * nz + zz) * CHUNKS + h], z * nx + (x + j) % nx
        )

    def got(b, h):
        ag_copy(b, h, ag_up.at[0], (me + 1) % n).wait_recv()

    def forward(k, h):
        below, above = z - k, z + k

        @pl.when(below >= 0)
        def _():
            @pl.when(k > 0)
            def _():
                got(below * nx + x, h)

            @pl.when(z < nz - 1)
            def _():
                up_copy(below, h).start()

            @pl.when((k == 0) & (z > 0))
            def _():
                down_copy(below, h).start()

            for j in range(1, nx):
                x_copy(below, h, j).start()

        @pl.when((k > 0) & (above < nz))
        def _():
            got(above * nx + x, h)

            @pl.when(z > 0)
            def _():
                down_copy(above, h).start()

            for j in range(1, nx):
                x_copy(above, h, j).start()

    lanes = lax.broadcasted_iota(jnp.int32, (own_rows, 128), 1)
    column_ids = lax.broadcasted_iota(jnp.int32, (own_rows, columns), 1).astype(f32)

    def score(b):
        s = jnp.dot(rows[b], mat[...], preferred_element_type=f32) + bias_ref[...]
        scores[b] = s
        m = jnp.max(s, axis=1, keepdims=True)
        t = jnp.sum(jnp.exp(s - m), axis=1, keepdims=True)
        hit = column_ids == tw[b][:, 0:1]
        g = jnp.sum(jnp.where(hit, s, 0.0), axis=1, keepdims=True)
        statc[b] = jnp.where(lanes == 0, m, jnp.where(lanes == 1, t, g))

    def gather_step(k, _):
        @pl.when(k < nz)
        def _():
            for h in range(CHUNKS):
                forward(k, h)

        @pl.when(k == 0)
        def _():
            mat_copy.wait()

        def visit(t, _):
            i, j = t % 2, t // 2
            kk = jnp.where(j == 0, k, k - 1)
            zz = z + (2 * i - 1) * kk
            b = zz * nx + (x + j) % nx

            @pl.when((kk >= 0) & (zz >= 0) & (zz < nz) & ((kk > 0) | (i == 0)))
            def _():
                @pl.when(j > 0)
                def _():
                    for h in range(CHUNKS):
                        got(b, h)

                score(b)

            return 0

        lax.fori_loop(0, 2 * nx, visit, 0)
        return 0

    lax.fori_loop(0, nz + 1, gather_step, 0)

    lined = jnp.transpose(statc[...].reshape(total, 128))
    groups = total // 128
    packed = jnp.concatenate(
        [lined[s : s + 1, c * 128 : (c + 1) * 128] for s in range(3) for c in range(groups)], axis=0
    )
    stats_out[...] = packed
    stats_all[0] = packed

    def stat_copy(k):
        return pltpu.make_async_remote_copy(
            src_ref=stats_out, dst_ref=stats_all.at[k], send_sem=st_s.at[k], recv_sem=st_r.at[k],
            device_id={"vp": (me + k) % n}, device_id_type=MESH,
        )

    def stat_start(k, _):
        stat_copy(k).start()
        return 0

    lax.fori_loop(1, n, stat_start, 0)

    def turn(c, _):
        at = pl.ds(pl.multiple_of(c * 128, 128), 128)
        rowst[at, :] = jnp.transpose(rows[:, :, at].astype(f32).reshape(total, 128)).astype(bf16)
        return 0

    lax.fori_loop(0, width // 128, turn, 0)

    def stat_wait(k, _):
        stat_copy(k).wait()
        return 0

    lax.fori_loop(1, n, stat_wait, 0)
    every = stats_all[...]
    maxima = every[:, 0:groups, :]
    peak = jnp.max(maxima, axis=0)
    summed = jnp.sum(every[:, groups : 2 * groups, :] * jnp.exp(maxima - peak[None]), axis=0)
    hit_score = jnp.sum(every[:, 2 * groups : 3 * groups, :], axis=0)
    log_total = peak + jnp.log(summed)
    loss = log_total - hit_score + penalty * log_total * log_total

    def one_row(v):
        return jnp.concatenate([v[c : c + 1, :] for c in range(groups)], axis=1)

    stacked = jnp.concatenate(
        [one_row(log_total), one_row(loss), jnp.zeros((126, total), f32)], axis=0
    )
    colv[...] = jnp.transpose(stacked).reshape(n, own_rows, 128)

    def grads(b):
        lt = colv[b][:, 0:1]
        w = tw[b][:, 1:2]
        hit = column_ids == tw[b][:, 0:1]
        probs = jnp.exp(scores[b] - lt)
        sg[b] = (
            w * ((1.0 + 2.0 * penalty * lt) * probs - jnp.where(hit, 1.0, 0.0))
        ).astype(bf16)

    def lane_part(h):
        return pl.ds(h * half, half)

    def x_send(slot, j, h):
        return pltpu.make_async_remote_copy(
            src_ref=xsend.at[slot, :, lane_part(h)], dst_ref=xrecv.at[slot, :, lane_part(h)],
            send_sem=xs.at[slot * CHUNKS + h], recv_sem=xr.at[slot * CHUNKS + h],
            device_id={"vp": z * nx + (x + j) % nx}, device_id_type=MESH,
        )

    def row_part(u, _):
        j = (u // (2 * nz) + 1) % nx
        k = nz - 1 - (u // 2) % nz
        i = u % 2
        zz = z + (2 * i - 1) * k

        @pl.when((zz >= 0) & (zz < nz) & ((k > 0) | (i == 0)))
        def _():
            b = zz * nx + (x + j) % nx
            grads(b)
            p = lax.dot_general(sg[b], mat[...], (((1,), (1,)), ((), ())), preferred_element_type=f32)

            @pl.when(j > 0)
            def _():
                slot = (j - 1) * nz + zz
                xsend[slot] = p.astype(bf16)
                for h in range(CHUNKS):
                    x_send(slot, j, h).start()

            @pl.when(j == 0)
            def _():
                part[zz] = p

        return 0

    def flat_grad():
        if own_rows % 16 == 0:
            return sg[...].reshape(total, columns)
        return sg[...].astype(f32).reshape(total, columns).astype(bf16)

    def vocab_part(d):
        at = pl.ds(pl.multiple_of(d * out_rows, out_rows), out_rows)
        return jnp.dot(rowst[at, :], flat_grad(), preferred_element_type=f32)

    def core_copy(q):
        return pltpu.make_async_remote_copy(
            src_ref=csend.at[q], dst_ref=crecv.at[q], send_sem=cs.at[q], recv_sem=cr.at[q],
            device_id={"dp": partner}, device_id_type=MESH,
        )

    def y_copy(q):
        return pltpu.make_async_remote_copy(
            src_ref=ysend.at[q], dst_ref=yrecv.at[q], send_sem=ys.at[q], recv_sem=yr.at[q],
            device_id={"dp": ((y + 1 + q) % ny) * 2 + core}, device_id_type=MESH,
        )

    def core_part(q, _):
        csend[q] = vocab_part(((y + 1 + q) % ny) * 2 + 1 - core).astype(bf16)
        core_copy(q).start()
        return 0

    def own_part(q, _):
        own[...] = vocab_part(((y + 1 + q) % ny) * 2 + core)
        core_copy(q).wait_recv()

        @pl.when(q < ny - 1)
        def _():
            slot = jnp.minimum(q, max(ny - 2, 0))
            ysend[slot] = (own[...] + crecv[q].astype(f32)).astype(bf16)
            y_copy(slot).start()

        @pl.when(q == ny - 1)
        def _():
            vout_ref[...] = own[...] + crecv[q].astype(f32)

        return 0

    def z_copy(i, zz, h):
        return pltpu.make_async_remote_copy(
            src_ref=zsend.at[zz, :, lane_part(h)], dst_ref=zrecv.at[i * nz + zz, :, lane_part(h)],
            send_sem=zs.at[zz * CHUNKS + h], recv_sem=zr.at[(i * nz + zz) * CHUNKS + h],
            device_id={"vp": (z + 2 * i - 1) * nx + x}, device_id_type=MESH,
        )

    def add_x(zz, h):
        for j in range(1, nx):
            slot = (j - 1) * nz + zz
            x_send(slot, j, h).wait_recv()
            part[zz, :, lane_part(h)] += xrecv[slot, :, lane_part(h)].astype(f32)

    def add_z(i, zz, h):
        z_copy(i, zz, h).wait_recv()
        part[zz, :, lane_part(h)] += zrecv[i * nz + zz, :, lane_part(h)].astype(f32)

    def chain(k):
        def one(i, h):
            zz = z + (2 * i - 1) * k

            @pl.when((zz >= 0) & (zz < nz))
            def _():
                add_x(zz, h)

                @pl.when(((i == 1) & (z > 0)) | ((i == 0) & (z < nz - 1)))
                def _():
                    add_z(i, zz, h)

                zsend[zz, :, lane_part(h)] = part[zz, :, lane_part(h)].astype(bf16)
                z_copy(i, zz, h).start()

        for h in range(CHUNKS):
            lax.fori_loop(0, 2, lambda i, c, h=h: (one(i, h), c)[1], 0)

    def chain_at(s, _):
        chain(nz - 1 - s)
        return 0

    lax.fori_loop(0, 2 * nz * (nx - 1), row_part, 0)
    lax.fori_loop(2 * nz * (nx - 1), 2 * nz * nx, row_part, 0)
    lax.fori_loop(0, ny, core_part, 0)
    lax.fori_loop(0, 1, chain_at, 0)
    lax.fori_loop(0, ny, own_part, 0)
    lax.fori_loop(1, nz - 1, chain_at, 0)

    own_col = jnp.concatenate([colv[me], jnp.zeros((128 - own_rows, 128), f32)], axis=0)
    loss_ref[...] = jnp.transpose(own_col)[1:2, :own_rows]

    for h in range(CHUNKS):
        add_x(z, h)

        @pl.when(z > 0)
        def _():
            add_z(1, z, h)

        @pl.when(z < nz - 1)
        def _():
            add_z(0, z, h)

    hid = hid_ref[...].astype(f32)
    inverse_rms = lax.rsqrt(jnp.mean(hid * hid, axis=-1, keepdims=True) + epsilon)
    unit = hid * inverse_rms
    scaled = gain_ref[...] * part[z]
    ngrad_ref[...] = inverse_rms * (scaled - unit * jnp.mean(scaled * unit, axis=-1, keepdims=True))

    for q in range(ny - 1):
        y_copy(q).wait_recv()
        vout_ref[...] += yrecv[q].astype(f32)

    def drain(zz, _):
        for h in range(CHUNKS):
            @pl.when((zz <= z) & (z < nz - 1))
            def _():
                up_copy(zz, h).wait_send()

            @pl.when((zz >= z) & (z > 0))
            def _():
                down_copy(zz, h).wait_send()

            for j in range(1, nx):
                x_copy(zz, h, j).wait_send()

            for j in range(1, nx):
                x_send((j - 1) * nz + zz, j, h).wait_send()

            @pl.when(zz > z)
            def _():
                z_copy(1, zz, h).wait_send()

            @pl.when(zz < z)
            def _():
                z_copy(0, zz, h).wait_send()

        return 0

    lax.fori_loop(0, nz, drain, 0)
    for q in range(ny):
        core_copy(q).wait_send()
    for q in range(ny - 1):
        y_copy(q).wait_send()


def solution(mesh):
    n, dp = mesh.shape["vp"], mesh.shape["dp"]
    ny = dp // 2
    nx = 1
    while (2 * nx) ** 2 <= n and n % (2 * nx) == 0:
        nx *= 2
    nz = n // nx

    def local(hidden_rows, norm_gain, vocab_matrix, vocab_bias, targets, loss_weight):
        own_rows, _, width = hidden_rows.shape
        columns = vocab_matrix.shape[1]
        total = n * own_rows
        out_rows = width // dp
        f32, bf16 = jnp.float32, jnp.bfloat16
        vmem = pl.BlockSpec(memory_space=pltpu.VMEM)
        dma = pltpu.SemaphoreType.DMA
        others = max(ny - 1, 1)
        xslots = max((nx - 1) * nz, 1)
        block = (own_rows, width)
        losses, norm_grad, vocab_grad = pl.pallas_call(
            functools.partial(kernel, n, nx, ny),
            out_shape=(
                jax.ShapeDtypeStruct((1, own_rows), f32),
                jax.ShapeDtypeStruct(block, f32),
                jax.ShapeDtypeStruct((out_rows, columns), f32),
            ),
            in_specs=[vmem, vmem, pl.BlockSpec(memory_space=pl.ANY), vmem, vmem, vmem],
            out_specs=(vmem, vmem, vmem),
            scratch_shapes=[
                pltpu.VMEM((n,) + block, bf16),
                pltpu.VMEM((width, columns), bf16),
                pltpu.VMEM((n, own_rows, columns), f32),
                pltpu.VMEM((n, own_rows, columns), bf16),
                pltpu.VMEM((nz,) + block, f32),
                pltpu.VMEM((xslots,) + block, bf16),
                pltpu.VMEM((xslots,) + block, bf16),
                pltpu.VMEM((nz,) + block, bf16),
                pltpu.VMEM((2 * nz,) + block, bf16),
                pltpu.VMEM((width, total), bf16),
                pltpu.VMEM((ny, out_rows, columns), bf16),
                pltpu.VMEM((ny, out_rows, columns), bf16),
                pltpu.VMEM((others, out_rows, columns), bf16),
                pltpu.VMEM((others, out_rows, columns), bf16),
                pltpu.VMEM((out_rows, columns), f32),
                pltpu.VMEM((n, own_rows, 128), f32),
                pltpu.VMEM((3 * (total // 128), 128), f32),
                pltpu.VMEM((n, 3 * (total // 128), 128), f32),
                pltpu.VMEM((n, own_rows, 128), f32),
                pltpu.VMEM((n, own_rows, 128), f32),
                dma,
                dma((n * CHUNKS,)),
                dma((nz * CHUNKS,)),
                dma((nz * CHUNKS,)),
                dma((xslots * CHUNKS,)),
                dma((n,)),
                dma((n,)),
                dma((xslots * CHUNKS,)),
                dma((xslots * CHUNKS,)),
                dma((nz * CHUNKS,)),
                dma((2 * nz * CHUNKS,)),
                dma((ny,)),
                dma((ny,)),
                dma((others,)),
                dma((others,)),
            ],
            compiler_params=pltpu.CompilerParams(
                collective_id=0, has_side_effects=True, vmem_limit_bytes=60 * 1024 * 1024
            ),
        )(
            hidden_rows.reshape(block),
            norm_gain.reshape(1, width),
            vocab_matrix,
            vocab_bias.reshape(1, columns),
            targets.reshape(1, total),
            loss_weight.reshape(1, total),
        )
        return losses.reshape(own_rows, 1), norm_grad.reshape(own_rows, 1, width), vocab_grad

    in_specs = (P("vp", "dp", None), P(), P(None, "vp"), P("vp"), P(None, "dp"), P(None, "dp"))
    out_specs = (P("vp", "dp"), P("vp", "dp", None), P("dp", "vp"))
    return jax.shard_map(local, mesh=mesh, in_specs=in_specs, out_specs=out_specs, check_vma=False)
```

```python
import functools

import jax
import jax.numpy as jnp
from jax import lax
from jax.experimental import pallas as pl
from jax.experimental.pallas import tpu as pltpu
from jax.sharding import PartitionSpec as P

epsilon = 1e-06
penalty = 0.005
MESH = pl.DeviceIdType.MESH
CHUNKS = 2
PIECES = 3


def kernel(
    n, nx, ny,
    hid_ref, gain_ref, mat_hbm, bias_ref, tgt_ref, wgt_ref,
    loss_ref, ngrad_ref, vout_ref,
    rows, mat, scores, sg, part, xsend, xrecv, zsend, zrecv,
    rowst, csend, crecv, ysend, yrecv, own, statc, stats_out, stats_all, colv, tw,
    mat_sem, ag_r, ag_up, ag_dn, ag_x, st_s, st_r, xs, xr, zs, zr, cs, cr, ys, yr,
):
    nz = n // nx
    me = lax.axis_index("vp")
    dme = lax.axis_index("dp")
    z, x = me // nx, me % nx
    y, core = dme // 2, dme % 2
    own_rows, width = hid_ref.shape
    columns = mat.shape[1]
    total = n * own_rows
    half = width // CHUNKS
    out_rows = vout_ref.shape[0]
    f32, bf16 = jnp.float32, jnp.bfloat16

    mat_copy = pltpu.make_async_copy(mat_hbm, mat, mat_sem)
    mat_copy.start()

    barrier = pltpu.get_barrier_semaphore()

    def greet(k, _):
        pl.semaphore_signal(barrier, inc=1, device_id={"vp": (me + k) % n}, device_id_type=MESH)
        return 0

    lax.fori_loop(1, n, greet, 0)
    partner = y * 2 + 1 - core
    pl.semaphore_signal(barrier, inc=1, device_id={"dp": partner}, device_id_type=MESH)
    for q in range(ny - 1):
        pl.semaphore_signal(
            barrier, inc=1, device_id={"dp": ((y + 1 + q) % ny) * 2 + core}, device_id_type=MESH
        )

    hid = hid_ref[...].astype(f32)
    inverse_rms = lax.rsqrt(jnp.mean(hid * hid, axis=-1, keepdims=True) + epsilon)
    rows[me] = (hid * inverse_rms * gain_ref[...]).astype(bf16)
    turned = jnp.transpose(
        jnp.concatenate(
            [
                (tgt_ref[...] - me * columns).astype(f32),
                wgt_ref[...],
                jnp.zeros((126, total), f32),
            ],
            axis=0,
        )
    )
    tw[...] = turned.reshape(n, own_rows, 128)
    pl.semaphore_wait(barrier, n - 1 + ny)

    units = width // 128
    last = max(1, units * 3 // 16)
    first = (units - last) // 2
    starts = (0, first * 128, (units - last) * 128)
    sizes = (first * 128, (units - last - first) * 128, last * 128)
    direct, across = (0, 1), 2

    def ag_copy(b, h, send_sem, target):
        piece = rows.at[b, :, pl.ds(starts[h], sizes[h])]
        return pltpu.make_async_remote_copy(
            src_ref=piece, dst_ref=piece, send_sem=send_sem, recv_sem=ag_r.at[b * PIECES + h],
            device_id={"vp": target}, device_id_type=MESH,
        )

    def block_of(zz, j):
        return zz * nx + (x + j) % nx

    def up_copy(zz, h, j=0):
        at = (j * nz + zz) * PIECES + h
        return ag_copy(block_of(zz, j), h, ag_up.at[at], (z + 1) * nx + x)

    def down_copy(zz, h, j=0):
        at = (j * nz + zz) * PIECES + h
        return ag_copy(block_of(zz, j), h, ag_dn.at[at], (z - 1) * nx + x)

    def x_copy(zz, h, j):
        return ag_copy(
            zz * nx + x, h, ag_x.at[((j - 1) * nz + zz) * PIECES + h], z * nx + (x + j) % nx
        )

    def got(b, h):
        ag_copy(b, h, ag_up.at[0], (me + 1) % n).wait_recv()

    def forward(k, h, j=0):
        below, above = z - k, z + k

        def cross(zz):
            if h != across:
                for to in range(1, nx):
                    x_copy(zz, h, to).start()

        @pl.when((k >= 0) & (below >= 0))
        def _():
            if j > 0:
                got(block_of(below, j), h)
            else:
                @pl.when(k > 0)
                def _():
                    got(block_of(below, j), h)

            @pl.when(z < nz - 1)
            def _():
                up_copy(below, h, j).start()

            @pl.when((k == 0) & (z > 0))
            def _():
                down_copy(below, h, j).start()

            cross(below)

        @pl.when((k > 0) & (above < nz))
        def _():
            got(block_of(above, j), h)

            @pl.when(z > 0)
            def _():
                down_copy(above, h, j).start()

            cross(above)

    lanes = lax.broadcasted_iota(jnp.int32, (own_rows, 128), 1)
    column_ids = lax.broadcasted_iota(jnp.int32, (own_rows, columns), 1).astype(f32)

    def score(b):
        s = jnp.dot(rows[b], mat[...], preferred_element_type=f32) + bias_ref[...]
        scores[b] = s
        m = jnp.max(s, axis=1, keepdims=True)
        t = jnp.sum(jnp.exp(s - m), axis=1, keepdims=True)
        hit = column_ids == tw[b][:, 0:1]
        g = jnp.sum(jnp.where(hit, s, 0.0), axis=1, keepdims=True)
        statc[b] = jnp.where(lanes == 0, m, jnp.where(lanes == 1, t, g))

    def gather_step(k, _):
        @pl.when(k == 0)
        def _():
            for j in range(1, nx):
                x_copy(z, across, j).start()

        for j in range(1, nx):
            forward(k - 1, across, j)
        for h in direct:
            forward(k, h)
        forward(k, across)

        @pl.when(k == 0)
        def _():
            mat_copy.wait()

        def visit(t, _):
            i, j = t % 2, t // 2
            kk = jnp.where(j == 0, k, k - 1)
            zz = z + (2 * i - 1) * kk
            b = zz * nx + (x + j) % nx

            @pl.when((kk >= 0) & (zz >= 0) & (zz < nz) & ((kk > 0) | (i == 0)))
            def _():
                @pl.when(j > 0)
                def _():
                    for h in direct:
                        got(b, h)

                score(b)

            return 0

        lax.fori_loop(0, 2 * nx, visit, 0)
        return 0

    lax.fori_loop(0, nz + 1, gather_step, 0)

    lined = jnp.transpose(statc[...].reshape(total, 128))
    groups = total // 128
    packed = jnp.concatenate(
        [lined[s : s + 1, c * 128 : (c + 1) * 128] for s in range(3) for c in range(groups)], axis=0
    )
    stats_out[...] = packed
    stats_all[0] = packed

    def stat_copy(k):
        return pltpu.make_async_remote_copy(
            src_ref=stats_out, dst_ref=stats_all.at[k], send_sem=st_s.at[k], recv_sem=st_r.at[k],
            device_id={"vp": (me + k) % n}, device_id_type=MESH,
        )

    def stat_start(k, _):
        stat_copy(k).start()
        return 0

    lax.fori_loop(1, n, stat_start, 0)

    def turn(c, _):
        at = pl.ds(pl.multiple_of(c * 128, 128), 128)
        rowst[at, :] = jnp.transpose(rows[:, :, at].astype(f32).reshape(total, 128)).astype(bf16)
        return 0

    lax.fori_loop(0, width // 128, turn, 0)

    def stat_wait(k, _):
        stat_copy(k).wait()
        return 0

    lax.fori_loop(1, n, stat_wait, 0)
    every = stats_all[...]
    maxima = every[:, 0:groups, :]
    peak = jnp.max(maxima, axis=0)
    summed = jnp.sum(every[:, groups : 2 * groups, :] * jnp.exp(maxima - peak[None]), axis=0)
    hit_score = jnp.sum(every[:, 2 * groups : 3 * groups, :], axis=0)
    log_total = peak + jnp.log(summed)
    loss = log_total - hit_score + penalty * log_total * log_total

    def one_row(v):
        return jnp.concatenate([v[c : c + 1, :] for c in range(groups)], axis=1)

    stacked = jnp.concatenate(
        [one_row(log_total), one_row(loss), jnp.zeros((126, total), f32)], axis=0
    )
    colv[...] = jnp.transpose(stacked).reshape(n, own_rows, 128)

    def grads(b):
        lt = colv[b][:, 0:1]
        w = tw[b][:, 1:2]
        hit = column_ids == tw[b][:, 0:1]
        probs = jnp.exp(scores[b] - lt)
        sg[b] = (
            w * ((1.0 + 2.0 * penalty * lt) * probs - jnp.where(hit, 1.0, 0.0))
        ).astype(bf16)

    def lane_part(h):
        return pl.ds(h * half, half)

    def x_send(slot, j, h):
        return pltpu.make_async_remote_copy(
            src_ref=xsend.at[slot, :, lane_part(h)], dst_ref=xrecv.at[slot, :, lane_part(h)],
            send_sem=xs.at[slot * CHUNKS + h], recv_sem=xr.at[slot * CHUNKS + h],
            device_id={"vp": z * nx + (x + j) % nx}, device_id_type=MESH,
        )

    def row_part(u, _):
        j = (u // (2 * nz) + 1) % nx
        k = nz - 1 - (u // 2) % nz
        i = u % 2
        zz = z + (2 * i - 1) * k

        @pl.when((zz >= 0) & (zz < nz) & ((k > 0) | (i == 0)))
        def _():
            b = zz * nx + (x + j) % nx
            grads(b)
            p = lax.dot_general(sg[b], mat[...], (((1,), (1,)), ((), ())), preferred_element_type=f32)

            @pl.when(j > 0)
            def _():
                slot = (j - 1) * nz + zz
                xsend[slot] = p.astype(bf16)
                for h in range(CHUNKS):
                    x_send(slot, j, h).start()

            @pl.when(j == 0)
            def _():
                part[zz] = p

        return 0

    def flat_grad():
        if own_rows % 16 == 0:
            return sg[...].reshape(total, columns)
        return sg[...].astype(f32).reshape(total, columns).astype(bf16)

    def vocab_part(d):
        at = pl.ds(pl.multiple_of(d * out_rows, out_rows), out_rows)
        return jnp.dot(rowst[at, :], flat_grad(), preferred_element_type=f32)

    def core_copy(q):
        return pltpu.make_async_remote_copy(
            src_ref=csend.at[q], dst_ref=crecv.at[q], send_sem=cs.at[q], recv_sem=cr.at[q],
            device_id={"dp": partner}, device_id_type=MESH,
        )

    def y_copy(q):
        return pltpu.make_async_remote_copy(
            src_ref=ysend.at[q], dst_ref=yrecv.at[q], send_sem=ys.at[q], recv_sem=yr.at[q],
            device_id={"dp": ((y + 1 + q) % ny) * 2 + core}, device_id_type=MESH,
        )

    def core_part(q, _):
        csend[q] = vocab_part(((y + 1 + q) % ny) * 2 + 1 - core).astype(bf16)
        core_copy(q).start()
        return 0

    def own_part(q, _):
        own[...] = vocab_part(((y + 1 + q) % ny) * 2 + core)
        core_copy(q).wait_recv()

        @pl.when(q < ny - 1)
        def _():
            slot = jnp.minimum(q, max(ny - 2, 0))
            ysend[slot] = (own[...] + crecv[q].astype(f32)).astype(bf16)
            y_copy(slot).start()

        @pl.when(q == ny - 1)
        def _():
            vout_ref[...] = own[...] + crecv[q].astype(f32)

        return 0

    def z_copy(i, zz, h):
        return pltpu.make_async_remote_copy(
            src_ref=zsend.at[zz, :, lane_part(h)], dst_ref=zrecv.at[i * nz + zz, :, lane_part(h)],
            send_sem=zs.at[zz * CHUNKS + h], recv_sem=zr.at[(i * nz + zz) * CHUNKS + h],
            device_id={"vp": (z + 2 * i - 1) * nx + x}, device_id_type=MESH,
        )

    def add_x(zz, h):
        for j in range(1, nx):
            slot = (j - 1) * nz + zz
            x_send(slot, j, h).wait_recv()
            part[zz, :, lane_part(h)] += xrecv[slot, :, lane_part(h)].astype(f32)

    def add_z(i, zz, h):
        z_copy(i, zz, h).wait_recv()
        part[zz, :, lane_part(h)] += zrecv[i * nz + zz, :, lane_part(h)].astype(f32)

    def chain(k):
        def one(i, h):
            zz = z + (2 * i - 1) * k

            @pl.when((zz >= 0) & (zz < nz))
            def _():
                add_x(zz, h)

                @pl.when(((i == 1) & (z > 0)) | ((i == 0) & (z < nz - 1)))
                def _():
                    add_z(i, zz, h)

                zsend[zz, :, lane_part(h)] = part[zz, :, lane_part(h)].astype(bf16)
                z_copy(i, zz, h).start()

        for h in range(CHUNKS):
            lax.fori_loop(0, 2, lambda i, c, h=h: (one(i, h), c)[1], 0)

    def chain_at(s, _):
        chain(nz - 1 - s)
        return 0

    lax.fori_loop(0, 2 * nz * (nx - 1), row_part, 0)
    lax.fori_loop(2 * nz * (nx - 1), 2 * nz * nx, row_part, 0)
    lax.fori_loop(0, ny, core_part, 0)
    lax.fori_loop(0, 1, chain_at, 0)
    lax.fori_loop(0, ny, own_part, 0)
    lax.fori_loop(1, nz - 1, chain_at, 0)

    own_col = jnp.concatenate([colv[me], jnp.zeros((128 - own_rows, 128), f32)], axis=0)
    loss_ref[...] = jnp.transpose(own_col)[1:2, :own_rows]

    for h in range(CHUNKS):
        add_x(z, h)

        @pl.when(z > 0)
        def _():
            add_z(1, z, h)

        @pl.when(z < nz - 1)
        def _():
            add_z(0, z, h)

    hid = hid_ref[...].astype(f32)
    inverse_rms = lax.rsqrt(jnp.mean(hid * hid, axis=-1, keepdims=True) + epsilon)
    unit = hid * inverse_rms
    scaled = gain_ref[...] * part[z]
    ngrad_ref[...] = inverse_rms * (scaled - unit * jnp.mean(scaled * unit, axis=-1, keepdims=True))

    for q in range(ny - 1):
        y_copy(q).wait_recv()
        vout_ref[...] += yrecv[q].astype(f32)

    def drain(zz, _):
        for h, j in [(h, 0) for h in range(PIECES)] + [(across, j) for j in range(1, nx)]:
            @pl.when((zz <= z) & (z < nz - 1))
            def _():
                up_copy(zz, h, j).wait_send()

            @pl.when((zz >= z) & (z > 0))
            def _():
                down_copy(zz, h, j).wait_send()

        for j in range(1, nx):
            for h in direct:
                x_copy(zz, h, j).wait_send()

            @pl.when(zz == z)
            def _():
                x_copy(zz, across, j).wait_send()

        for h in range(CHUNKS):
            for j in range(1, nx):
                x_send((j - 1) * nz + zz, j, h).wait_send()

            @pl.when(zz > z)
            def _():
                z_copy(1, zz, h).wait_send()

            @pl.when(zz < z)
            def _():
                z_copy(0, zz, h).wait_send()

        return 0

    lax.fori_loop(0, nz, drain, 0)
    for q in range(ny):
        core_copy(q).wait_send()
    for q in range(ny - 1):
        y_copy(q).wait_send()


def solution(mesh):
    n, dp = mesh.shape["vp"], mesh.shape["dp"]
    ny = dp // 2
    nx = 1
    while (2 * nx) ** 2 <= n and n % (2 * nx) == 0:
        nx *= 2
    nz = n // nx

    def local(hidden_rows, norm_gain, vocab_matrix, vocab_bias, targets, loss_weight):
        own_rows, _, width = hidden_rows.shape
        columns = vocab_matrix.shape[1]
        total = n * own_rows
        out_rows = width // dp
        f32, bf16 = jnp.float32, jnp.bfloat16
        vmem = pl.BlockSpec(memory_space=pltpu.VMEM)
        dma = pltpu.SemaphoreType.DMA
        others = max(ny - 1, 1)
        xslots = max((nx - 1) * nz, 1)
        block = (own_rows, width)
        losses, norm_grad, vocab_grad = pl.pallas_call(
            functools.partial(kernel, n, nx, ny),
            out_shape=(
                jax.ShapeDtypeStruct((1, own_rows), f32),
                jax.ShapeDtypeStruct(block, f32),
                jax.ShapeDtypeStruct((out_rows, columns), f32),
            ),
            in_specs=[vmem, vmem, pl.BlockSpec(memory_space=pl.ANY), vmem, vmem, vmem],
            out_specs=(vmem, vmem, vmem),
            scratch_shapes=[
                pltpu.VMEM((n,) + block, bf16),
                pltpu.VMEM((width, columns), bf16),
                pltpu.VMEM((n, own_rows, columns), f32),
                pltpu.VMEM((n, own_rows, columns), bf16),
                pltpu.VMEM((nz,) + block, f32),
                pltpu.VMEM((xslots,) + block, bf16),
                pltpu.VMEM((xslots,) + block, bf16),
                pltpu.VMEM((nz,) + block, bf16),
                pltpu.VMEM((2 * nz,) + block, bf16),
                pltpu.VMEM((width, total), bf16),
                pltpu.VMEM((ny, out_rows, columns), bf16),
                pltpu.VMEM((ny, out_rows, columns), bf16),
                pltpu.VMEM((others, out_rows, columns), bf16),
                pltpu.VMEM((others, out_rows, columns), bf16),
                pltpu.VMEM((out_rows, columns), f32),
                pltpu.VMEM((n, own_rows, 128), f32),
                pltpu.VMEM((3 * (total // 128), 128), f32),
                pltpu.VMEM((n, 3 * (total // 128), 128), f32),
                pltpu.VMEM((n, own_rows, 128), f32),
                pltpu.VMEM((n, own_rows, 128), f32),
                dma,
                dma((n * PIECES,)),
                dma((n * PIECES,)),
                dma((n * PIECES,)),
                dma((xslots * PIECES,)),
                dma((n,)),
                dma((n,)),
                dma((xslots * CHUNKS,)),
                dma((xslots * CHUNKS,)),
                dma((nz * CHUNKS,)),
                dma((2 * nz * CHUNKS,)),
                dma((ny,)),
                dma((ny,)),
                dma((others,)),
                dma((others,)),
            ],
            compiler_params=pltpu.CompilerParams(
                collective_id=0, has_side_effects=True, vmem_limit_bytes=60 * 1024 * 1024
            ),
        )(
            hidden_rows.reshape(block),
            norm_gain.reshape(1, width),
            vocab_matrix,
            vocab_bias.reshape(1, columns),
            targets.reshape(1, total),
            loss_weight.reshape(1, total),
        )
        return losses.reshape(own_rows, 1), norm_grad.reshape(own_rows, 1, width), vocab_grad

    in_specs = (P("vp", "dp", None), P(), P(None, "vp"), P("vp"), P(None, "dp"), P(None, "dp"))
    out_specs = (P("vp", "dp"), P("vp", "dp", None), P("dp", "vp"))
    return jax.shard_map(local, mesh=mesh, in_specs=in_specs, out_specs=out_specs, check_vma=False)
```
